32 devices in a mesh: sp: 8 (over z, y), tp: 4 (over x, core).
Axes of the slice: x: 2, y: 2, z: 4, core: 2. Of those that a mesh axis runs over, the one named last changes fastest.
Arguments:
- tokens: bfloat16 [4, 1024, 2048], P(None, 'sp'), may hold values from -6 to 6
- next_tokens: bfloat16 [4, 2048], replicated, may hold values from -6 to 6
- w_query: bfloat16 [2048, 2048], P(None, 'tp'), may hold values from -0.125 to 0.125
- w_key: bfloat16 [2048, 2048], P(None, 'tp'), may hold values from -0.125 to 0.125
- w_value: bfloat16 [2048, 2048], P(None, 'tp'), may hold values from -0.125 to 0.125
- w_in_gate: bfloat16 [2048, 8], replicated, may hold values from -0.125 to 0.125
- w_forget_gate: bfloat16 [2048, 8], replicated, may hold values from -0.125 to 0.125
- forget_bias: float32 [8], replicated, may hold values from 3 to 14
- extra_decay: float32 [8, 4, 1024], P('tp', None, 'sp'), may hold values from -0.5509766 to 0
- w_out: bfloat16 [2048, 2048], P('tp'), may hold values from -0.125 to 0.125
Outputs:
- memory: bfloat16 [8, 1024, 256], P('tp', 'sp')
- normalizer: float32 [8, 1024], P('tp', 'sp')
- stabilizer: float32 [4, 8], P(None, 'tp')
- read: bfloat16 [4, 2048], replicated
The draws below stay inside these ranges and needn't reach their ends.
All inputs are finite; a program needn't handle non-finite values.
Results may differ from the reference program's by a relative error of at most 0.024.
Values may be sent and summed in bfloat16 or wider, within the bound.
A program may use at most 64 MiB of HBM per device.

```python
import jax
import jax.numpy as jnp
from jax import lax

D = 2048
H = 8
HD = 256
SEQS = 4
TOK_DEV = 512
LENGTH = 1024
N_TP = 4


def draw_forget_bias(key, part):
    first, second, third = jax.random.split(key, 3)
    order = jax.random.permutation(first, H)
    slow = order < H // 2
    high = jax.random.uniform(second, (H,), jnp.float32, minval=11.0, maxval=14.0)
    low = jax.random.uniform(third, (H,), jnp.float32, minval=3.0, maxval=5.0)
    return jnp.where(slow, high, low)


def draw_extra_decay(key, part):
    first, second, third = jax.random.split(key, 3)
    span = TOK_DEV // SEQS
    blocks = LENGTH // span
    rate = jnp.exp(jax.random.uniform(first, (H, SEQS, blocks), jnp.float32, minval=jnp.log(0.2), maxval=0.0)) / LENGTH
    base = -jnp.repeat(rate, span, axis=2)
    hits = jax.random.randint(second, (H, SEQS, LENGTH), 0, LENGTH) < 3
    drop = jax.random.uniform(third, (H, SEQS, LENGTH), jnp.float32, minval=0.22, maxval=0.5)
    return base - jnp.where(hits, drop, 0.0)


def steps_of(rng, shape, shards, low, largest):
    loudness, own = 1.0, jax.random.fold_in(rng, 6)
    for dim, parts in shards:
        steps = jnp.exp(jax.random.uniform(jax.random.fold_in(own, dim), (parts,), jnp.float32, low / len(shards), largest / len(shards)))
        loudness = loudness * jnp.repeat(steps, shape[dim] // parts).reshape([-1 if axis == dim else 1 for axis in range(len(shape))])
    return loudness


def normal_values(stream_key, extent, deviation, most, shards=(), held_as=jnp.bfloat16):
    result = jax.random.normal(stream_key, extent, jnp.float32) * deviation
    if len(shards) > 0:
        result = steps_of(stream_key, extent, shards, -0.22, 0.18) * result
    return jnp.clip(result, min=-most, max=most).astype(held_as)


def setup_inputs(seed: int = 0) -> dict:
    key_list = jax.random.split(jax.random.key(seed), 11)
    return {
        "tokens": normal_values(key_list[0], (SEQS, LENGTH, D), 1.0, 6.0, ((1, 8),)),
        "next_tokens": normal_values(key_list[1], (SEQS, D), 1.0, 6.0),
        "w_query": normal_values(key_list[2], (D, H * HD), D ** -0.5, 0.125, ((1, 4),)),
        "w_key": normal_values(key_list[3], (D, H * HD), D ** -0.5, 0.125, ((1, 4),)),
        "w_value": normal_values(key_list[4], (D, H * HD), D ** -0.5, 0.125, ((1, 4),)),
        "w_in_gate": normal_values(key_list[5], (D, H), D ** -0.5, 0.125),
        "w_forget_gate": normal_values(key_list[6], (D, H), D ** -0.5, 0.125),
        "forget_bias": draw_forget_bias(jax.random.fold_in(key_list[10], 71), 0),
        "extra_decay": draw_extra_decay(jax.random.fold_in(key_list[10], 71), 0),
        "w_out": normal_values(key_list[9], (H * HD, D), (H * HD) ** -0.5, 0.125, ((0, 4),)),
    }


def reference(tokens, next_tokens, w_query, w_key, w_value, w_in_gate, w_forget_gate, forget_bias, extra_decay, w_out):
    scale = HD ** -0.5
    flat = tokens.reshape(SEQS * LENGTH, D)
    keys = jnp.dot(flat, w_key, preferred_element_type=jnp.float32).astype(jnp.bfloat16)
    values = jnp.dot(flat, w_value, preferred_element_type=jnp.float32).astype(jnp.bfloat16)
    log_in = jnp.dot(flat, w_in_gate, preferred_element_type=jnp.float32).reshape(SEQS, LENGTH, H)
    log_forget = jax.nn.log_sigmoid(jnp.dot(flat, w_forget_gate, preferred_element_type=jnp.float32) + forget_bias).reshape(SEQS, LENGTH, H) + jnp.transpose(extra_decay, (1, 2, 0))
    prefix = jnp.cumsum(log_forget, axis=1)
    total = prefix[:, -1]
    score = total[:, None, :] - prefix + log_in
    stabilizer = jnp.maximum(total, jnp.max(score, axis=1))
    weight = jnp.exp(score - stabilizer[:, None, :]) * scale
    keys4 = keys.reshape(SEQS, LENGTH, H, HD)
    values4 = values.reshape(SEQS, LENGTH, H, HD)

    def one_prompt(items):
        key_rows, value_rows, weight_rows = items
        weighted = (key_rows.astype(jnp.float32) * weight_rows[:, :, None]).astype(jnp.bfloat16)
        state = jnp.einsum('lhd,lhe->hde', weighted.astype(jnp.float32), value_rows.astype(jnp.float32))
        norm_state = jnp.sum(weighted.astype(jnp.float32), axis=0)
        return state, norm_state

    state, norm_state = lax.map(one_prompt, (keys4, values4, weight))
    memory = jnp.transpose(state, (1, 0, 2, 3)).reshape(H, SEQS * HD, HD).astype(jnp.bfloat16)
    normalizer = jnp.transpose(norm_state, (1, 0, 2)).reshape(H, SEQS * HD)
    query = jnp.dot(next_tokens, w_query, preferred_element_type=jnp.float32).astype(jnp.bfloat16).astype(jnp.float32).reshape(SEQS, H, HD)
    new_key = jnp.dot(next_tokens, w_key, preferred_element_type=jnp.float32).astype(jnp.bfloat16).astype(jnp.float32).reshape(SEQS, H, HD) * scale
    new_value = jnp.dot(next_tokens, w_value, preferred_element_type=jnp.float32).astype(jnp.bfloat16).astype(jnp.float32).reshape(SEQS, H, HD)
    new_in = jnp.dot(next_tokens, w_in_gate, preferred_element_type=jnp.float32)
    new_forget = jax.nn.log_sigmoid(jnp.dot(next_tokens, w_forget_gate, preferred_element_type=jnp.float32) + forget_bias)
    query_state = jnp.einsum('shd,shde->she', query, state, precision=lax.Precision.HIGHEST)
    query_norm = jnp.sum(query * norm_state, axis=-1)
    top = jnp.maximum(new_forget + stabilizer, new_in)
    keep = jnp.exp(new_forget + stabilizer - top)
    take = jnp.exp(new_in - top)
    qk = jnp.sum(query * new_key, axis=-1)
    numer = keep[:, :, None] * query_state + (take * qk)[:, :, None] * new_value
    denom = keep * query_norm + take * qk
    head_out = (numer / jnp.maximum(jnp.abs(denom), 1.0)[:, :, None]).astype(jnp.bfloat16)
    grouped = head_out.reshape(SEQS, N_TP, (H // N_TP) * HD).astype(jnp.float32)
    out_rows = w_out.reshape(N_TP, (H // N_TP) * HD, D).astype(jnp.float32)
    partial_sums = jnp.einsum('sgc,gcd->gsd', grouped, out_rows).astype(jnp.bfloat16)
    read = jnp.sum(partial_sums.astype(jnp.float32), axis=0).astype(jnp.bfloat16)
    return memory, normalizer, stabilizer, read
```

```python
import functools

import jax
import jax.numpy as jnp
from jax import lax
from jax.experimental import pallas as pl
from jax.experimental.pallas import tpu as pltpu
from jax.sharding import PartitionSpec as P

HD = 256
LANES = 128
F32 = jnp.float32
BF16 = jnp.bfloat16
HIGHEST = lax.Precision.HIGHEST


def log_sigmoid(x):
    return jnp.minimum(x, 0.0) - jnp.log1p(jnp.exp(-jnp.abs(x)))


def dot(a, b, dims=((1,), (0,)), precision=None):
    return lax.dot_general(a, b, (dims, ((), ())), precision=precision, preferred_element_type=F32)


def kernel(
    seqs, span, heads, sp, tp,
    tokens, next_tokens, w_query, w_key, w_value, w_in, w_forget, bias, decay, w_out,
    mem_out, norm_out, stab_out, read_out,
    x, wq, wk, wv, wo, wg, bias_wide, decay_wide, stats, state, pair_send, pair_recv,
    far_send, far_recv, slots, parts,
    load_sem, stat_ss, stat_rs, pair_ss, pair_rs, far_ss, far_rs, slot_ss, slot_rs, part_ss, part_rs,
):
    me = lax.axis_index("sp")
    me_tp = lax.axis_index("tp")
    count = seqs * span
    rows = seqs * HD // sp
    groups = sp // 2
    group = me // 2
    side = lax.rem(me, 2)
    partner = me + 1 - 2 * side
    scale = HD ** (-0.5)

    loads = []

    def load(src, dst):
        loads.append(pltpu.make_async_copy(src, dst, load_sem.at[len(loads)]))
        loads[-1].start()
        return loads[-1]

    load_x = load(tokens, x.at[pl.ds(0, count)])
    load_k = [None] * heads
    load_v = [None] * heads
    for h in range(heads):
        cols = pl.ds(h * HD, HD)
        load_k[h] = load(w_key.at[:, cols], wk.at[h])
        load_v[h] = load(w_value.at[:, cols], wv.at[h])
    load_q = load(w_query, wq)
    load_o = load(w_out, wo)

    barrier = pltpu.get_barrier_semaphore()
    for k in range(1, sp):
        pl.semaphore_signal(barrier, inc=1, device_id={"sp": lax.rem(me + k, sp)})
    for k in range(1, tp):
        pl.semaphore_signal(barrier, inc=1, device_id={"tp": lax.rem(me_tp + k, tp)})

    def send(src, dst, ss, rs, where):
        copy = pltpu.make_async_remote_copy(
            src_ref=src, dst_ref=dst, send_sem=ss, recv_sem=rs, device_id=where
        )
        copy.start()
        return copy

    x[pl.ds(count, 16), :] = jnp.zeros((16, x.shape[1]), BF16)
    x[pl.ds(count, seqs), :] = next_tokens[...]
    wg[...] = jnp.zeros_like(wg)
    width = w_in.shape[1]
    wg[:, 0:width] = w_in[...]
    wg[:, LANES : LANES + width] = w_forget[...]
    bias_wide[...] = jnp.zeros_like(bias_wide)
    bias_wide[0:1, 0:width] = bias[...]
    decay_wide[...] = jnp.zeros_like(decay_wide)
    for p in range(seqs):
        for h in range(heads):
            decay_wide[p, h : h + 1, :] = decay[h, p : p + 1, :]

    load_x.wait()
    gates = dot(x[...], wg[...])
    shift = lax.rem(LANES - me_tp * heads, LANES)
    log_in = pltpu.roll(gates[:, :LANES], shift, 1)
    forget = pltpu.roll(log_sigmoid(gates[:, LANES:] + bias_wide[0:1, :]), shift, 1)
    after = (
        lax.broadcasted_iota(jnp.int32, (span, span), 1)
        > lax.broadcasted_iota(jnp.int32, (span, span), 0)
    ).astype(F32)
    weight = []
    for p in range(seqs):
        block = forget[p * span : (p + 1) * span] + decay_wide[p].T
        score = dot(after, block, precision=HIGHEST) + log_in[p * span : (p + 1) * span]
        peak = jnp.max(score, axis=0, keepdims=True)
        stats[0, p : p + 1, :] = jnp.sum(block, axis=0, keepdims=True)
        stats[0, seqs + p : seqs + p + 1, :] = peak
        weight.append(jnp.exp(score - peak) * scale)
    weight = jnp.concatenate(weight, axis=0)
    new_in = log_in[count : count + seqs]
    new_forget = forget[count : count + seqs]

    pl.semaphore_wait(barrier, sp - 1 + tp - 1)
    stat_copies = [
        send(stats.at[0], stats.at[k], stat_ss.at[k], stat_rs.at[k], {"sp": lax.rem(me + k, sp)})
        for k in range(1, sp)
    ]

    order = list(range(1, groups)) + [0]
    if groups > 2:
        order = [groups // 2] + [k for k in order if k != groups // 2]
    mask = (
        lax.broadcasted_iota(jnp.int32, (16, count), 1) // span
        == lax.broadcasted_iota(jnp.int32, (16, count), 0)
    )
    pick = jnp.where(mask, 1.0, 0.0).astype(BF16)
    factor = None
    query = None
    pair_copies = {}
    new_keys, new_values, queries = [], [], []
    slot_copies = []

    for h in range(heads):
        load_k[h].wait()
        keys = dot(x[...], wk[h]).astype(BF16)
        load_v[h].wait()
        values = dot(x[...], wv[h]).astype(BF16)
        weighted = (keys[:count].astype(F32) * weight[:, h : h + 1]).astype(BF16)
        new_keys.append(keys[count : count + seqs].astype(F32) * scale)
        new_values.append(values[count : count + seqs].astype(F32))
        if factor is None:
            for copy in stat_copies:
                copy.wait()
            later = jnp.zeros((seqs, LANES), F32)
            stab = None
            here = later
            for s in range(sp - 1, -1, -1):
                slot = lax.rem(me - s + sp, sp)
                peak = stats[slot, seqs : 2 * seqs, :]
                total = stats[slot, 0:seqs, :]
                stab = later + peak if stab is None else jnp.maximum(stab, later + peak)
                here = jnp.where(me == s, later + peak, here)
                later = later + total
            stab = jnp.maximum(stab, later)
            factor = jnp.exp(here - stab)
            stab_out[...] = stab
        for p in range(seqs):
            part = slice(p * span, (p + 1) * span)
            block = dot(weighted[part], values[part], ((0,), (0,)))
            state[h, pl.ds(p * HD, HD), :] = block * factor[p : p + 1, h : h + 1]
        for k in order:
            owner = 2 * lax.rem(group + k, groups) + 1 - side
            start = pl.multiple_of(owner * rows, rows)
            pair_send[h, k] = state[h, pl.ds(start, rows), :].astype(BF16)
            i = h * groups + k
            pair_copies[h, k] = send(
                pair_send.at[h, k], pair_recv.at[h, k], pair_ss.at[i], pair_rs.at[i],
                {"sp": partner},
            )
        if query is None:
            load_q.wait()
            query = dot(x[pl.ds(count, 16), :], wq[...]).astype(BF16)
        q = query[:, h * HD : (h + 1) * HD]
        queries.append(q[:seqs].astype(F32))
        reach = jnp.where(mask, dot(q, weighted, ((1,), (1,))), 0.0)
        high = reach.astype(BF16)
        low = (reach - high.astype(F32)).astype(BF16)
        product = dot(high, values[:count]) + dot(low, values[:count])
        norm = dot(pick, weighted)
        slots[0, 0, h] = product[:seqs] * factor[:, h : h + 1]
        slots[0, 1, h] = norm[:seqs] * factor[:, h : h + 1]

    slot_copies = [
        send(slots.at[0], slots.at[k], slot_ss.at[k], slot_rs.at[k], {"sp": lax.rem(me + k, sp)})
        for k in range(1, sp)
    ]

    far_copies = {}

    def forward(h):
        for k in order:
            pair_copies[h, k].wait()
            if k == 0:
                continue
            to = lax.rem(group + k, groups)
            start = pl.multiple_of((2 * to + side) * rows, rows)
            far_send[h, k] = (
                state[h, pl.ds(start, rows), :] + pair_recv[h, k].astype(F32)
            ).astype(BF16)
            i = h * groups + k
            far_copies[h, k] = send(
                far_send.at[h, k], far_recv.at[h, k], far_ss.at[i], far_rs.at[i],
                {"sp": 2 * to + side},
            )

    forward(0)

    for copy in slot_copies:
        copy.wait()
    total = [[None] * heads for _ in range(2)]
    for s in range(sp):
        slot = lax.rem(me - s + sp, sp)
        for kind in range(2):
            for h in range(heads):
                term = slots[slot, kind, h]
                total[kind][h] = term if s == 0 else total[kind][h] + term
    top = jnp.maximum(new_forget + stab, new_in)
    keep = jnp.exp(new_forget + stab - top)
    take = jnp.exp(new_in - top)
    outs = []
    for h in range(heads):
        norm_out[h] = total[1][h]
        keep_h = keep[:, h : h + 1]
        taken = take[:, h : h + 1] * jnp.sum(queries[h] * new_keys[h], axis=1, keepdims=True)
        numer = keep_h * total[0][h] + taken * new_values[h]
        denom = keep_h * jnp.sum(queries[h] * total[1][h], axis=1, keepdims=True) + taken
        outs.append(numer / jnp.maximum(jnp.abs(denom), 1.0))
    load_o.wait()
    outs = jnp.concatenate(outs, axis=1) if heads > 1 else outs[0]
    parts[0] = dot(outs.astype(BF16), wo[...]).astype(BF16)
    part_copies = [
        send(
            parts.at[0], parts.at[k], part_ss.at[k], part_rs.at[k],
            {"tp": lax.rem(me_tp + k, tp)},
        )
        for k in range(1, tp)
    ]
    for h in range(1, heads):
        forward(h)
    for copy in part_copies:
        copy.wait()
    read = None
    for t in range(tp):
        term = parts[lax.rem(me_tp - t + tp, tp)].astype(F32)
        read = term if read is None else read + term
    read_out[...] = read.astype(BF16)

    start = pl.multiple_of(me * rows, rows)
    for h in range(heads):
        mine = state[h, pl.ds(start, rows), :] + pair_recv[h, 0].astype(F32)
        for k in order[:-1]:
            far_copies[h, k].wait()
            mine = mine + far_recv[h, k].astype(F32)
        mem_out[h] = mine.astype(BF16)


def per_device(
    sp, tp,
    tokens, next_tokens, w_query, w_key, w_value, w_in_gate, w_forget_gate, forget_bias,
    extra_decay, w_out,
):
    seqs, span, model = tokens.shape
    heads = w_key.shape[1] // HD
    rows = seqs * HD // sp
    groups = sp // 2
    count = seqs * span
    any_spec = pl.BlockSpec(memory_space=pl.ANY)
    vmem = pl.BlockSpec(memory_space=pltpu.VMEM)
    dma = pltpu.SemaphoreType.DMA
    memory, norm, stab, read = pl.pallas_call(
        functools.partial(kernel, seqs, span, heads, sp, tp),
        out_shape=(
            jax.ShapeDtypeStruct((heads, rows, HD), BF16),
            jax.ShapeDtypeStruct((heads, seqs, HD), F32),
            jax.ShapeDtypeStruct((seqs, LANES), F32),
            jax.ShapeDtypeStruct((seqs, w_out.shape[1]), BF16),
        ),
        in_specs=[any_spec, vmem, any_spec, any_spec, any_spec, vmem, vmem, vmem, vmem, any_spec],
        out_specs=(vmem, vmem, vmem, vmem),
        scratch_shapes=[
            pltpu.VMEM((count + 16, model), BF16),
            pltpu.VMEM(w_query.shape, BF16),
            pltpu.VMEM((heads, model, HD), BF16),
            pltpu.VMEM((heads, model, HD), BF16),
            pltpu.VMEM(w_out.shape, BF16),
            pltpu.VMEM((model, 2 * LANES), BF16),
            pltpu.VMEM((8, LANES), F32),
            pltpu.VMEM((seqs, LANES, span), F32),
            pltpu.VMEM((sp, 2 * seqs, LANES), F32),
            pltpu.VMEM((heads, seqs * HD, HD), F32),
            pltpu.VMEM((heads, groups, rows, HD), BF16),
            pltpu.VMEM((heads, groups, rows, HD), BF16),
            pltpu.VMEM((heads, groups, rows, HD), BF16),
            pltpu.VMEM((heads, groups, rows, HD), BF16),
            pltpu.VMEM((sp, 2, heads, seqs, HD), F32),
            pltpu.VMEM((tp, seqs, w_out.shape[1]), BF16),
            dma((3 + 2 * heads,)),
            dma((sp,)),
            dma((sp,)),
            dma((heads * groups,)),
            dma((heads * groups,)),
            dma((heads * groups,)),
            dma((heads * groups,)),
            dma((sp,)),
            dma((sp,)),
            dma((tp,)),
            dma((tp,)),
        ],
        compiler_params=pltpu.CompilerParams(
            collective_id=0, has_side_effects=True, vmem_limit_bytes=56 * 1024 * 1024
        ),
    )(
        tokens.reshape(count, model), next_tokens, w_query, w_key, w_value, w_in_gate,
        w_forget_gate, forget_bias.reshape(1, -1), extra_decay, w_out,
    )
    start = lax.axis_index("sp") * rows
    norm_rows = lax.dynamic_slice_in_dim(norm.reshape(heads, seqs * HD), start, rows, 1)
    return memory, norm_rows, stab[:, :heads], read


def solution(mesh):
    placed = (
        P(None, "sp", None),
        P(),
        P(None, "tp"),
        P(None, "tp"),
        P(None, "tp"),
        P(),
        P(),
        P(),
        P("tp", None, "sp"),
        P("tp", None),
    )
    return jax.shard_map(
        functools.partial(per_device, mesh.shape["sp"], mesh.shape["tp"]),
        mesh=mesh,
        in_specs=placed,
        out_specs=(P("tp", "sp", None), P("tp", "sp"), P(None, "tp"), P()),
        check_vma=False,
    )
```

```python
import functools

import jax
import jax.numpy as jnp
from jax import lax
from jax.experimental import pallas as pl
from jax.experimental.pallas import tpu as pltpu
from jax.sharding import PartitionSpec as P

HD = 256
LANES = 128
VMEM_LIMIT = 63 * 1024 * 1024
F32 = jnp.float32
BF16 = jnp.bfloat16
HIGHEST = lax.Precision.HIGHEST


def log_sigmoid(x):
    return jnp.minimum(x, 0.0) - jnp.log1p(jnp.exp(-jnp.abs(x)))


def dot(a, b, dims=((1,), (0,)), precision=None):
    return lax.dot_general(a, b, (dims, ((), ())), precision=precision, preferred_element_type=F32)


def kernel(
    seqs, span, heads, sp, tp,
    tokens, next_tokens, w_query, w_key, w_value, w_in, w_forget, bias, decay, w_out,
    mem_out, norm_out, stab_out, read_out,
    x, wq, wk, wv, wo, wg, bias_wide, decay_wide, stats, state, pair_send, pair_recv,
    far_send, far_recv, slots, parts,
    load_sem, stat_ss, stat_rs, pair_ss, pair_rs, far_ss, far_rs, slot_ss, slot_rs, part_ss, part_rs,
):
    me = lax.axis_index("sp")
    me_tp = lax.axis_index("tp")
    count = seqs * span
    rows = seqs * HD // sp
    groups = sp // 2
    group = me // 2
    side = lax.rem(me, 2)
    partner = me + 1 - 2 * side
    scale = HD ** (-0.5)

    loads = []

    def load(src, dst):
        loads.append(pltpu.make_async_copy(src, dst, load_sem.at[len(loads)]))
        loads[-1].start()
        return loads[-1]

    load_x = load(tokens, x.at[pl.ds(0, count)])
    load_k = [None] * heads
    load_v = [None] * heads
    for h in range(heads):
        cols = pl.ds(h * HD, HD)
        load_k[h] = load(w_key.at[:, cols], wk.at[h])
        load_v[h] = load(w_value.at[:, cols], wv.at[h])
    load_q = load(w_query, wq)
    load_o = load(w_out, wo)

    barrier = pltpu.get_barrier_semaphore()
    for k in range(1, sp):
        pl.semaphore_signal(barrier, inc=1, device_id={"sp": lax.rem(me + k, sp)})
    for k in range(1, tp):
        pl.semaphore_signal(barrier, inc=1, device_id={"tp": lax.rem(me_tp + k, tp)})

    def send(src, dst, ss, rs, where):
        copy = pltpu.make_async_remote_copy(
            src_ref=src, dst_ref=dst, send_sem=ss, recv_sem=rs, device_id=where
        )
        copy.start()
        return copy

    x[pl.ds(count, 16), :] = jnp.zeros((16, x.shape[1]), BF16)
    x[pl.ds(count, seqs), :] = next_tokens[...]
    wg[...] = jnp.zeros_like(wg)
    width = w_in.shape[0]
    wg[0:width, :] = w_in[...]
    wg[LANES : LANES + width, :] = w_forget[...]
    bias_wide[...] = jnp.zeros_like(bias_wide)
    bias_wide[0:1, 0:width] = bias[...]
    decay_wide[...] = jnp.zeros_like(decay_wide)
    for p in range(seqs):
        for h in range(heads):
            decay_wide[p, h : h + 1, :] = decay[h, p : p + 1, :]

    load_x.wait()
    gates = dot(x[...], wg[...], ((1,), (1,)))
    shift = lax.rem(LANES - me_tp * heads, LANES)
    log_in = pltpu.roll(gates[:, :LANES], shift, 1)
    forget = pltpu.roll(log_sigmoid(gates[:, LANES:] + bias_wide[0:1, :]), shift, 1)
    after = (
        lax.broadcasted_iota(jnp.int32, (span, span), 1)
        > lax.broadcasted_iota(jnp.int32, (span, span), 0)
    ).astype(F32)
    weight = []
    for p in range(seqs):
        block = forget[p * span : (p + 1) * span] + decay_wide[p].T
        score = dot(after, block, precision=HIGHEST) + log_in[p * span : (p + 1) * span]
        peak = jnp.max(score, axis=0, keepdims=True)
        stats[0, p : p + 1, :] = jnp.sum(block, axis=0, keepdims=True)
        stats[0, seqs + p : seqs + p + 1, :] = peak
        weight.append(jnp.exp(score - peak) * scale)
    weight = jnp.concatenate(weight, axis=0)
    new_in = log_in[count : count + seqs]
    new_forget = forget[count : count + seqs]

    pl.semaphore_wait(barrier, sp - 1 + tp - 1)
    stat_copies = [
        send(stats.at[0], stats.at[k], stat_ss.at[k], stat_rs.at[k], {"sp": lax.rem(me + k, sp)})
        for k in range(1, sp)
    ]

    order = list(range(1, groups)) + [0]
    if groups > 2:
        order = [groups // 2] + [k for k in order if k != groups // 2]
    mask = (
        lax.broadcasted_iota(jnp.int32, (16, count), 1) // span
        == lax.broadcasted_iota(jnp.int32, (16, count), 0)
    )
    pick = jnp.where(mask, 1.0, 0.0).astype(BF16)
    factor = None
    query = None
    pair_copies = {}
    new_keys, new_values, queries = [], [], []

    for h in range(heads):
        load_k[h].wait()
        keys = dot(x[...], wk[h]).astype(BF16)
        load_v[h].wait()
        values = dot(x[...], wv[h]).astype(BF16)
        weighted = (keys[:count].astype(F32) * weight[:, h : h + 1]).astype(BF16)
        new_keys.append(keys[count : count + seqs].astype(F32) * scale)
        new_values.append(values[count : count + seqs].astype(F32))
        if factor is None:
            for copy in stat_copies:
                copy.wait()
            later = jnp.zeros((seqs, LANES), F32)
            stab = None
            here = later
            for s in range(sp - 1, -1, -1):
                slot = lax.rem(me - s + sp, sp)
                peak = stats[slot, seqs : 2 * seqs, :]
                total = stats[slot, 0:seqs, :]
                stab = later + peak if stab is None else jnp.maximum(stab, later + peak)
                here = jnp.where(me == s, later + peak, here)
                later = later + total
            stab = jnp.maximum(stab, later)
            factor = jnp.exp(here - stab)
            stab_out[...] = stab

        def states():
            for p in range(seqs):
                part = slice(p * span, (p + 1) * span)
                block = dot(weighted[part], values[part], ((0,), (0,)))
                state[h, pl.ds(p * HD, HD), :] = block * factor[p : p + 1, h : h + 1]
            for k in order:
                owner = 2 * lax.rem(group + k, groups) + 1 - side
                start = pl.multiple_of(owner * rows, rows)
                pair_send[h, k] = state[h, pl.ds(start, rows), :].astype(BF16)
                i = h * groups + k
                pair_copies[h, k] = send(
                    pair_send.at[h, k], pair_recv.at[h, k], pair_ss.at[i], pair_rs.at[i],
                    {"sp": partner},
                )

        if h < heads - 1:
            states()
        if query is None:
            load_q.wait()
            query = dot(x[pl.ds(count, 16), :], wq[...]).astype(BF16)
        q = query[:, h * HD : (h + 1) * HD]
        queries.append(q[:seqs].astype(F32))
        reach = jnp.where(mask, dot(q, weighted, ((1,), (1,))), 0.0)
        high = reach.astype(BF16)
        low = (reach - high.astype(F32)).astype(BF16)
        product = dot(high, values[:count]) + dot(low, values[:count])
        norm = dot(pick, weighted)
        slots[0, 0, h] = product[:seqs] * factor[:, h : h + 1]
        slots[0, 1, h] = norm[:seqs] * factor[:, h : h + 1]
        if h == heads - 1:
            slot_copies = [
                send(
                    slots.at[0], slots.at[k], slot_ss.at[k], slot_rs.at[k],
                    {"sp": lax.rem(me + k, sp)},
                )
                for k in range(1, sp)
            ]
            states()

    far_copies = {}

    def forward(h):
        for k in order:
            pair_copies[h, k].wait()
            if k == 0:
                continue
            to = lax.rem(group + k, groups)
            start = pl.multiple_of((2 * to + side) * rows, rows)
            far_send[h, k] = (
                state[h, pl.ds(start, rows), :] + pair_recv[h, k].astype(F32)
            ).astype(BF16)
            i = h * groups + k
            far_copies[h, k] = send(
                far_send.at[h, k], far_recv.at[h, k], far_ss.at[i], far_rs.at[i],
                {"sp": 2 * to + side},
            )

    forward(0)

    for copy in slot_copies:
        copy.wait()
    total = [[None] * heads for _ in range(2)]
    for s in range(sp):
        slot = lax.rem(me - s + sp, sp)
        for kind in range(2):
            for h in range(heads):
                term = slots[slot, kind, h]
                total[kind][h] = term if s == 0 else total[kind][h] + term
    top = jnp.maximum(new_forget + stab, new_in)
    keep = jnp.exp(new_forget + stab - top)
    take = jnp.exp(new_in - top)
    outs = []
    for h in range(heads):
        mine_at = lax.broadcasted_iota(jnp.int32, (seqs, HD), 0) == me * rows // HD
        row = jnp.sum(jnp.where(mine_at, total[1][h], 0.0), axis=0, keepdims=True)
        turn = lax.rem(HD - lax.rem(me * rows, HD), HD)
        if rows < HD:
            row = pltpu.roll(jnp.broadcast_to(row, (8, HD)), turn, 1)[0:1, :rows]
        norm_out[h : h + 1, :] = row
        keep_h = keep[:, h : h + 1]
        taken = take[:, h : h + 1] * jnp.sum(queries[h] * new_keys[h], axis=1, keepdims=True)
        numer = keep_h * total[0][h] + taken * new_values[h]
        denom = keep_h * jnp.sum(queries[h] * total[1][h], axis=1, keepdims=True) + taken
        outs.append(numer / jnp.maximum(jnp.abs(denom), 1.0))
    load_o.wait()
    outs = jnp.concatenate(outs, axis=1) if heads > 1 else outs[0]
    parts[0] = dot(outs.astype(BF16), wo[...]).astype(BF16)
    part_copies = [
        send(
            parts.at[0], parts.at[k], part_ss.at[k], part_rs.at[k],
            {"tp": lax.rem(me_tp + k, tp)},
        )
        for k in range(1, tp)
    ]
    for h in range(1, heads):
        forward(h)
    for copy in part_copies:
        copy.wait()
    read = None
    for t in range(tp):
        term = parts[lax.rem(me_tp - t + tp, tp)].astype(F32)
        read = term if read is None else read + term
    read_out[...] = read.astype(BF16)

    start = pl.multiple_of(me * rows, rows)
    for h in range(heads):
        mine = state[h, pl.ds(start, rows), :] + pair_recv[h, 0].astype(F32)
        for k in order[:-1]:
            far_copies[h, k].wait()
            mine = mine + far_recv[h, k].astype(F32)
        mem_out[h] = mine.astype(BF16)


def finish(memory, norm, stab, read, memory_out, norm_out, stab_out, read_out):
    memory_out[...] = memory[...]
    norm_out[...] = norm[...]
    heads, seqs = stab_out.shape
    wide = jnp.concatenate([stab[...], jnp.zeros((8 - seqs, LANES), F32)], axis=0)
    stab_out[...] = wide.T[:heads, :seqs]
    read_out[...] = read[...]


def per_device(
    sp, tp,
    tokens, next_tokens, w_query, w_key, w_value, w_in_gate, w_forget_gate, forget_bias,
    extra_decay, w_out,
):
    seqs, span, model = tokens.shape
    heads = w_key.shape[1] // HD
    rows = seqs * HD // sp
    groups = sp // 2
    count = seqs * span
    any_spec = pl.BlockSpec(memory_space=pltpu.HBM)
    vmem = pl.BlockSpec(memory_space=pltpu.VMEM)
    dma = pltpu.SemaphoreType.DMA
    memory, norm, stab, read = pl.pallas_call(
        functools.partial(kernel, seqs, span, heads, sp, tp),
        out_shape=(
            jax.ShapeDtypeStruct((heads, rows, HD), BF16),
            jax.ShapeDtypeStruct((heads, rows), F32),
            jax.ShapeDtypeStruct((seqs, LANES), F32),
            jax.ShapeDtypeStruct((seqs, w_out.shape[1]), BF16),
        ),
        in_specs=[any_spec, vmem, any_spec, any_spec, any_spec, vmem, vmem, vmem, vmem, any_spec],
        out_specs=(vmem, vmem, vmem, vmem),
        scratch_shapes=[
            pltpu.VMEM((count + 16, model), BF16),
            pltpu.VMEM(w_query.shape, BF16),
            pltpu.VMEM((heads, model, HD), BF16),
            pltpu.VMEM((heads, model, HD), BF16),
            pltpu.VMEM(w_out.shape, BF16),
            pltpu.VMEM((2 * LANES, model), BF16),
            pltpu.VMEM((8, LANES), F32),
            pltpu.VMEM((seqs, LANES, span), F32),
            pltpu.VMEM((sp, 2 * seqs, LANES), F32),
            pltpu.VMEM((heads, seqs * HD, HD), F32),
            pltpu.VMEM((heads, groups, rows, HD), BF16),
            pltpu.VMEM((heads, groups, rows, HD), BF16),
            pltpu.VMEM((heads, groups, rows, HD), BF16),
            pltpu.VMEM((heads, groups, rows, HD), BF16),
            pltpu.VMEM((sp, 2, heads, seqs, HD), F32),
            pltpu.VMEM((tp, seqs, w_out.shape[1]), BF16),
            dma((3 + 2 * heads,)),
            dma((sp,)),
            dma((sp,)),
            dma((heads * groups,)),
            dma((heads * groups,)),
            dma((heads * groups,)),
            dma((heads * groups,)),
            dma((sp,)),
            dma((sp,)),
            dma((tp,)),
            dma((tp,)),
        ],
        compiler_params=pltpu.CompilerParams(
            collective_id=0, has_side_effects=True, vmem_limit_bytes=VMEM_LIMIT
        ),
    )(
        tokens.reshape(count, model), next_tokens, w_query, w_key, w_value, w_in_gate.T,
        w_forget_gate.T, forget_bias.reshape(1, -1), extra_decay, w_out,
    )
    memory, norm, stab, read = pl.pallas_call(
        finish,
        out_shape=(
            jax.ShapeDtypeStruct(memory.shape, BF16),
            jax.ShapeDtypeStruct(norm.shape, F32),
            jax.ShapeDtypeStruct((heads, seqs), F32),
            jax.ShapeDtypeStruct(read.shape, BF16),
        ),
        in_specs=[vmem] * 4,
        out_specs=(vmem,) * 4,
        compiler_params=pltpu.CompilerParams(vmem_limit_bytes=VMEM_LIMIT),
    )(memory, norm, stab, read)
    return memory, norm, stab.T, read


def solution(mesh):
    placed = (
        P(None, "sp", None),
        P(),
        P(None, "tp"),
        P(None, "tp"),
        P(None, "tp"),
        P(),
        P(),
        P(),
        P("tp", None, "sp"),
        P("tp", None),
    )
    return jax.shard_map(
        functools.partial(per_device, mesh.shape["sp"], mesh.shape["tp"]),
        mesh=mesh,
        in_specs=placed,
        out_specs=(P("tp", "sp", None), P("tp", "sp"), P(None, "tp"), P()),
        check_vma=False,
    )
```

```python
import functools

import jax
import jax.numpy as jnp
from jax import lax
from jax.experimental import pallas as pl
from jax.experimental.pallas import tpu as pltpu
from jax.sharding import PartitionSpec as P

HD = 256
LANES = 128
VMEM_LIMIT = 63 * 1024 * 1024
F32 = jnp.float32
BF16 = jnp.bfloat16
HIGHEST = lax.Precision.HIGHEST


def log_sigmoid(x):
    return jnp.minimum(x, 0.0) - jnp.log1p(jnp.exp(-jnp.abs(x)))


def dot(a, b, dims=((1,), (0,)), precision=None):
    return lax.dot_general(a, b, (dims, ((), ())), precision=precision, preferred_element_type=F32)


def kernel(
    seqs, span, heads, sp, tp,
    tokens, next_tokens, w_query, w_key, w_value, w_in, w_forget, bias, decay, w_out,
    mem_out, norm_out, stab_out, read_out,
    x, wq, wk, wv, wo, wg, bias_wide, decay_wide, stats, state, pair_send, pair_recv,
    far_send, far_recv, slots, parts,
    load_sem, stat_ss, stat_rs, pair_ss, pair_rs, far_ss, far_rs, slot_ss, slot_rs, part_ss, part_rs,
):
    me = lax.axis_index("sp")
    me_tp = lax.axis_index("tp")
    count = seqs * span
    rows = seqs * HD // sp
    groups = sp // 2
    group = me // 2
    side = lax.rem(me, 2)
    partner = me + 1 - 2 * side
    scale = HD ** (-0.5)

    barrier = pltpu.get_barrier_semaphore()
    for k in range(1, sp):
        pl.semaphore_signal(barrier, inc=1, device_id={"sp": lax.rem(me + k, sp)})
    for k in range(1, tp):
        pl.semaphore_signal(barrier, inc=1, device_id={"tp": lax.rem(me_tp + k, tp)})

    loads = []

    def load(src, dst):
        loads.append(pltpu.make_async_copy(src, dst, load_sem.at[len(loads)]))
        loads[-1].start()
        return loads[-1]

    load_x = load(tokens, x.at[pl.ds(0, count)])
    load_k = [None] * heads
    load_v = [None] * heads

    def load_head(h):
        cols = pl.ds(h * HD, HD)
        load_k[h] = load(w_key.at[:, cols], wk.at[h])
        load_v[h] = load(w_value.at[:, cols], wv.at[h])

    load_head(0)

    def send(src, dst, ss, rs, where):
        copy = pltpu.make_async_remote_copy(
            src_ref=src, dst_ref=dst, send_sem=ss, recv_sem=rs, device_id=where
        )
        copy.start()
        return copy

    x[pl.ds(count, 16), :] = jnp.zeros((16, x.shape[1]), BF16)
    x[pl.ds(count, seqs), :] = next_tokens[...]
    wg[...] = jnp.zeros_like(wg)
    width = w_in.shape[0]
    wg[0:width, :] = w_in[...]
    wg[LANES : LANES + width, :] = w_forget[...]
    bias_wide[...] = jnp.zeros_like(bias_wide)
    bias_wide[0:1, 0:width] = bias[...]
    decay_wide[...] = jnp.zeros_like(decay_wide)
    for p in range(seqs):
        for h in range(heads):
            decay_wide[p, h : h + 1, :] = decay[h, p : p + 1, :]

    load_x.wait()
    for h in range(1, heads):
        load_head(h)
    load_q = load(w_query, wq)
    load_o = load(w_out, wo)
    gates = dot(x[...], wg[...], ((1,), (1,)))
    shift = lax.rem(LANES - me_tp * heads, LANES)
    log_in = pltpu.roll(gates[:, :LANES], shift, 1)
    forget = pltpu.roll(log_sigmoid(gates[:, LANES:] + bias_wide[0:1, :]), shift, 1)
    after = (
        lax.broadcasted_iota(jnp.int32, (span, span), 1)
        > lax.broadcasted_iota(jnp.int32, (span, span), 0)
    ).astype(F32)
    weight = []
    for p in range(seqs):
        block = forget[p * span : (p + 1) * span] + decay_wide[p].T
        score = dot(after, block, precision=HIGHEST) + log_in[p * span : (p + 1) * span]
        peak = jnp.max(score, axis=0, keepdims=True)
        stats[0, p : p + 1, :] = jnp.sum(block, axis=0, keepdims=True)
        stats[0, seqs + p : seqs + p + 1, :] = peak
        weight.append(jnp.exp(score - peak) * scale)
    weight = jnp.concatenate(weight, axis=0)
    new_in = log_in[count : count + seqs]
    new_forget = forget[count : count + seqs]

    pl.semaphore_wait(barrier, sp - 1 + tp - 1)
    stat_copies = [
        send(stats.at[0], stats.at[k], stat_ss.at[k], stat_rs.at[k], {"sp": lax.rem(me + k, sp)})
        for k in range(1, sp)
    ]

    order = list(range(1, groups)) + [0]
    if groups > 2:
        order = [groups // 2] + [k for k in order if k != groups // 2]
    mask = (
        lax.broadcasted_iota(jnp.int32, (16, count), 1) // span
        == lax.broadcasted_iota(jnp.int32, (16, count), 0)
    )
    pick = jnp.where(mask, 1.0, 0.0).astype(BF16)
    query = None
    pair_copies = {}
    new_keys, new_values, queries, products, norms = [], [], [], [], []

    for h in range(heads):
        load_k[h].wait()
        keys = dot(x[...], wk[h]).astype(BF16)
        load_v[h].wait()
        values = dot(x[...], wv[h]).astype(BF16)
        weighted = (keys[:count].astype(F32) * weight[:, h : h + 1]).astype(BF16)
        new_keys.append(keys[count : count + seqs].astype(F32) * scale)
        new_values.append(values[count : count + seqs].astype(F32))

        def states():
            for p in range(seqs):
                part = slice(p * span, (p + 1) * span)
                block = dot(weighted[part], values[part], ((0,), (0,)))
                state[h, pl.ds(p * HD, HD), :] = block
            for k in order:
                owner = 2 * lax.rem(group + k, groups) + 1 - side
                start = pl.multiple_of(owner * rows, rows)
                pair_send[h, k] = state[h, pl.ds(start, rows), :].astype(BF16)
                i = h * groups + k
                pair_copies[h, k] = send(
                    pair_send.at[h, k], pair_recv.at[h, k], pair_ss.at[i], pair_rs.at[i],
                    {"sp": partner},
                )

        if h < heads - 1:
            states()
        if query is None:
            load_q.wait()
            query = dot(x[pl.ds(count, 16), :], wq[...]).astype(BF16)
        q = query[:, h * HD : (h + 1) * HD]
        queries.append(q[:seqs].astype(F32))
        reach = jnp.where(mask, dot(q, weighted, ((1,), (1,))), 0.0)
        high = reach.astype(BF16)
        low = (reach - high.astype(F32)).astype(BF16)
        product = dot(high, values[:count]) + dot(low, values[:count])
        norm = dot(pick, weighted)
        products.append(product[:seqs])
        norms.append(norm[:seqs])
        if h == heads - 1:
            for copy in stat_copies:
                copy.wait()
            later = jnp.zeros((seqs, LANES), F32)
            stab, here, there = None, later, later
            for s in range(sp - 1, -1, -1):
                slot = lax.rem(me - s + sp, sp)
                level = later + stats[slot, seqs : 2 * seqs, :]
                stab = level if stab is None else jnp.maximum(stab, level)
                here = jnp.where(me == s, level, here)
                there = jnp.where(partner == s, level, there)
                later = later + stats[slot, 0:seqs, :]
            stab = jnp.maximum(stab, later)
            factor = jnp.exp(here - stab)
            factor_there = jnp.exp(there - stab)
            stab_out[...] = stab
            for i in range(heads):
                slots[0, 0, i] = products[i] * factor[:, i : i + 1]
                slots[0, 1, i] = norms[i] * factor[:, i : i + 1]
            slot_copies = [
                send(
                    slots.at[0], slots.at[k], slot_ss.at[k], slot_rs.at[k],
                    {"sp": lax.rem(me + k, sp)},
                )
                for k in range(1, sp)
            ]
            states()

    far_copies = {}
    prompt = lax.broadcasted_iota(jnp.int32, (seqs, LANES), 0)

    def pair_sum(h, k, owner):
        at = prompt == owner * rows // HD
        mine = jnp.sum(jnp.where(at, factor, 0.0), axis=0, keepdims=True)[:, h : h + 1]
        other = jnp.sum(jnp.where(at, factor_there, 0.0), axis=0, keepdims=True)[:, h : h + 1]
        start = pl.multiple_of(owner * rows, rows)
        return state[h, pl.ds(start, rows), :] * mine + pair_recv[h, k].astype(F32) * other

    def forward(h):
        for k in order:
            pair_copies[h, k].wait()
            if k == 0:
                continue
            to = lax.rem(group + k, groups)
            far_send[h, k] = pair_sum(h, k, 2 * to + side).astype(BF16)
            i = h * groups + k
            far_copies[h, k] = send(
                far_send.at[h, k], far_recv.at[h, k], far_ss.at[i], far_rs.at[i],
                {"sp": 2 * to + side},
            )

    forward(0)

    for copy in slot_copies:
        copy.wait()
    total = [[None] * heads for _ in range(2)]
    for s in range(sp):
        slot = lax.rem(me - s + sp, sp)
        for kind in range(2):
            for h in range(heads):
                term = slots[slot, kind, h]
                total[kind][h] = term if s == 0 else total[kind][h] + term
    top = jnp.maximum(new_forget + stab, new_in)
    keep = jnp.exp(new_forget + stab - top)
    take = jnp.exp(new_in - top)
    outs = []
    for h in range(heads):
        mine_at = lax.broadcasted_iota(jnp.int32, (seqs, HD), 0) == me * rows // HD
        row = jnp.sum(jnp.where(mine_at, total[1][h], 0.0), axis=0, keepdims=True)
        turn = lax.rem(HD - lax.rem(me * rows, HD), HD)
        if rows < HD:
            row = pltpu.roll(jnp.broadcast_to(row, (8, HD)), turn, 1)[0:1, :rows]
        norm_out[h : h + 1, :] = row
        keep_h = keep[:, h : h + 1]
        taken = take[:, h : h + 1] * jnp.sum(queries[h] * new_keys[h], axis=1, keepdims=True)
        numer = keep_h * total[0][h] + taken * new_values[h]
        denom = keep_h * jnp.sum(queries[h] * total[1][h], axis=1, keepdims=True) + taken
        outs.append(numer / jnp.maximum(jnp.abs(denom), 1.0))
    load_o.wait()
    outs = jnp.concatenate(outs, axis=1) if heads > 1 else outs[0]
    parts[0] = dot(outs.astype(BF16), wo[...]).astype(BF16)
    part_copies = [
        send(
            parts.at[0], parts.at[k], part_ss.at[k], part_rs.at[k],
            {"tp": lax.rem(me_tp + k, tp)},
        )
        for k in range(1, tp)
    ]
    for h in range(1, heads):
        forward(h)
    for copy in part_copies:
        copy.wait()
    read = None
    for t in range(tp):
        term = parts[lax.rem(me_tp - t + tp, tp)].astype(F32)
        read = term if read is None else read + term
    read_out[...] = read.astype(BF16)

    for h in range(heads):
        mine = pair_sum(h, 0, me)
        for k in order[:-1]:
            far_copies[h, k].wait()
            mine = mine + far_recv[h, k].astype(F32)
        mem_out[h] = mine.astype(BF16)


def finish(memory, norm, stab, read, memory_out, norm_out, stab_out, read_out):
    memory_out[...] = memory[...]
    norm_out[...] = norm[...]
    heads, seqs = stab_out.shape
    wide = jnp.concatenate([stab[...], jnp.zeros((8 - seqs, LANES), F32)], axis=0)
    stab_out[...] = wide.T[:heads, :seqs]
    read_out[...] = read[...]


def per_device(
    sp, tp,
    tokens, next_tokens, w_query, w_key, w_value, w_in_gate, w_forget_gate, forget_bias,
    extra_decay, w_out,
):
    seqs, span, model = tokens.shape
    heads = w_key.shape[1] // HD
    rows = seqs * HD // sp
    groups = sp // 2
    count = seqs * span
    any_spec = pl.BlockSpec(memory_space=pltpu.HBM)
    vmem = pl.BlockSpec(memory_space=pltpu.VMEM)
    dma = pltpu.SemaphoreType.DMA
    memory, norm, stab, read = pl.pallas_call(
        functools.partial(kernel, seqs, span, heads, sp, tp),
        out_shape=(
            jax.ShapeDtypeStruct((heads, rows, HD), BF16),
            jax.ShapeDtypeStruct((heads, rows), F32),
            jax.ShapeDtypeStruct((seqs, LANES), F32),
            jax.ShapeDtypeStruct((seqs, w_out.shape[1]), BF16),
        ),
        in_specs=[any_spec, vmem, any_spec, any_spec, any_spec, vmem, vmem, vmem, vmem, any_spec],
        out_specs=(vmem, vmem, vmem, vmem),
        scratch_shapes=[
            pltpu.VMEM((count + 16, model), BF16),
            pltpu.VMEM(w_query.shape, BF16),
            pltpu.VMEM((heads, model, HD), BF16),
            pltpu.VMEM((heads, model, HD), BF16),
            pltpu.VMEM(w_out.shape, BF16),
            pltpu.VMEM((2 * LANES, model), BF16),
            pltpu.VMEM((8, LANES), F32),
            pltpu.VMEM((seqs, LANES, span), F32),
            pltpu.VMEM((sp, 2 * seqs, LANES), F32),
            pltpu.VMEM((heads, seqs * HD, HD), F32),
            pltpu.VMEM((heads, groups, rows, HD), BF16),
            pltpu.VMEM((heads, groups, rows, HD), BF16),
            pltpu.VMEM((heads, groups, rows, HD), BF16),
            pltpu.VMEM((heads, groups, rows, HD), BF16),
            pltpu.VMEM((sp, 2, heads, seqs, HD), F32),
            pltpu.VMEM((tp, seqs, w_out.shape[1]), BF16),
            dma((3 + 2 * heads,)),
            dma((sp,)),
            dma((sp,)),
            dma((heads * groups,)),
            dma((heads * groups,)),
            dma((heads * groups,)),
            dma((heads * groups,)),
            dma((sp,)),
            dma((sp,)),
            dma((tp,)),
            dma((tp,)),
        ],
        compiler_params=pltpu.CompilerParams(
            collective_id=0, has_side_effects=True, vmem_limit_bytes=VMEM_LIMIT
        ),
    )(
        tokens.reshape(count, model), next_tokens, w_query, w_key, w_value, w_in_gate.T,
        w_forget_gate.T, forget_bias.reshape(1, -1), extra_decay, w_out,
    )
    memory, norm, stab, read = pl.pallas_call(
        finish,
        out_shape=(
            jax.ShapeDtypeStruct(memory.shape, BF16),
            jax.ShapeDtypeStruct(norm.shape, F32),
            jax.ShapeDtypeStruct((heads, seqs), F32),
            jax.ShapeDtypeStruct(read.shape, BF16),
        ),
        in_specs=[vmem] * 4,
        out_specs=(vmem,) * 4,
        compiler_params=pltpu.CompilerParams(vmem_limit_bytes=VMEM_LIMIT),
    )(memory, norm, stab, read)
    return memory, norm, stab.T, read


def solution(mesh):
    placed = (
        P(None, "sp", None),
        P(),
        P(None, "tp"),
        P(None, "tp"),
        P(None, "tp"),
        P(),
        P(),
        P(),
        P("tp", None, "sp"),
        P("tp", None),
    )
    return jax.shard_map(
        functools.partial(per_device, mesh.shape["sp"], mesh.shape["tp"]),
        mesh=mesh,
        in_specs=placed,
        out_specs=(P("tp", "sp", None), P("tp", "sp"), P(None, "tp"), P()),
        check_vma=False,
    )
```
